32 devices in a mesh: pp: 4 (over z), fs: 4 (over y, x), tp: 2 (over core).
Axes of the slice: x: 2, y: 2, z: 4, core: 2. Of those that a mesh axis runs over, the one named last changes fastest.
Arguments:
- tokens: bfloat16 [4, 512, 1024], P('pp', 'fs', 'tp'), parts along dimension 1, may hold values from -640 to 640
- query_matrix: bfloat16 [4, 1024, 1024], P('pp', None, 'tp'), may hold values from -0.1875 to 0.1875
- key_matrix: bfloat16 [4, 1024, 1024], P('pp', None, 'tp'), may hold values from -0.1875 to 0.1875
- value_matrix: bfloat16 [4, 1024, 1024], P('pp', None, 'tp'), may hold values from -0.1875 to 0.1875
- output_gate_weight: bfloat16 [4, 1024, 1024], P('pp', None, 'tp'), may hold values from -0.1875 to 0.1875
- strength_weight: bfloat16 [4, 1024, 8], P('pp', None, 'tp'), may hold values from -0.1875 to 0.1875
- decay_input_weight: bfloat16 [4, 1024, 8], P('pp', None, 'tp'), may hold values from -0.1875 to 0.1875
- decay_scale_table: float32 [4, 8], P('pp', 'tp'), may hold values from 0.00078125 to 0.234375
- log_spike_decay: float32 [4, 128, 8], P('pp', None, 'tp'), may hold values from -2.1 to 0
- head_norm_gain: float32 [4, 1024], P('pp', 'tp'), may hold values from 0.1 to 1.9
- closing_norm_gain: float32 [1024], P('tp'), may hold values from 0.1 to 1.9
Outputs:
- normalized: bfloat16 [4, 512, 1024], P('pp', 'fs', 'tp'), parts along dimension 1
The draws below stay inside these ranges and needn't reach their ends.
There are 4 independent parts, one for each index of `fs`. The reference program is written for one: setup_inputs(seed, part) draws one part's arguments, and reference() takes and returns one part's arrays. A program takes and returns all parts, laid end to end along the dimension named above; an argument that names none is the same for every part. Nothing has to cross between parts.
All inputs are finite; a program needn't handle non-finite values.
Results may differ from the reference program's by a relative error of at most 0.012.
Values may be sent and summed in bfloat16 or wider, within the bound.
A program may use at most 64 MiB of HBM per device.

```python
import math
from functools import partial
import jax
import jax.numpy as jnp
from jax import lax

D = 1024
HEAD_TOTAL = 8
HEAD_DIM = 128
BLOCK = 64
SEQUENCE_LENGTH = 128
LAYER_TOTAL = 4
MICRO = 4


spike_count = 3


def draw_tokens(key, part):
    base_key, row_key = jax.random.split(jax.random.fold_in(key, 17), 2)
    column_ramp = jnp.exp(math.log(10.0) * jnp.arange(D, dtype=jnp.float32) / (D - 1))
    base_values = jnp.clip(jax.random.normal(base_key, (MICRO, SEQUENCE_LENGTH, D), jnp.float32), -4.0, 4.0)
    row_scale = jnp.exp(jax.random.uniform(row_key, (MICRO, SEQUENCE_LENGTH, 1), jnp.float32, 0.0, math.log(10.0)))
    return (base_values * row_scale * column_ramp).astype(jnp.bfloat16)


def draw_decay_scale_table(key, part):
    lower_rate = 0.3 / SEQUENCE_LENGTH
    upper_rate = 30.0 / SEQUENCE_LENGTH
    logged = jax.random.uniform(jax.random.fold_in(key, 23), (LAYER_TOTAL, HEAD_TOTAL), jnp.float32, math.log(lower_rate), math.log(upper_rate))
    return jnp.exp(logged)


def draw_log_spike_decay(key, part):
    position_random_key, layer_random_key = jax.random.split(jax.random.fold_in(key, 29))
    position_indices = jax.random.randint(position_random_key, (LAYER_TOTAL, spike_count, HEAD_TOTAL), 0, SEQUENCE_LENGTH)
    layer_indices = jnp.log(jax.random.uniform(layer_random_key, (LAYER_TOTAL, spike_count, HEAD_TOTAL), jnp.float32, 0.5, 0.8))
    hit_mask = (position_indices[:, :, None, :] == jnp.arange(SEQUENCE_LENGTH)[None, None, :, None]).astype(jnp.float32)
    return jnp.sum(hit_mask * layer_indices[:, :, None, :], axis=1)


def shard_levels(own_key, extent, cuts, least, top_value):
    level = 1.0
    for dim, shards_of in cuts:
        steps = jax.random.uniform(jax.random.fold_in(jax.random.fold_in(own_key, 6), dim), (shards_of,), jnp.float32, least / len(cuts), top_value / len(cuts))
        level = level * jnp.repeat(jnp.exp(steps), extent[dim] // shards_of).reshape((-1,) + (1,) * (len(extent) - 1 - dim))
    return level


def gaussian(own_key, extent, deviation, reach, shards=(), kind=jnp.bfloat16):
    factor_of = shard_levels(own_key, extent, shards, -0.22, 0.18) if shards else 1.0
    drawn = jax.random.normal(own_key, extent, jnp.float32) * deviation * factor_of
    return jnp.minimum(jnp.maximum(drawn, -reach), reach).astype(kind)


def setup_inputs(seed: int = 0, part: int = 0) -> dict:
    splits = jax.random.split(jax.random.key(seed), 12)
    part_splits = jax.random.split(jax.random.fold_in(splits[11], part), 12)
    return {
        "tokens": draw_tokens(jax.random.fold_in(jax.random.fold_in(splits[11], part), 71), part),
        "query_matrix": gaussian(splits[1], (LAYER_TOTAL, D, HEAD_TOTAL * HEAD_DIM), D ** -0.5, 0.1875, ((0, 4), (2, 2))),
        "key_matrix": gaussian(splits[2], (LAYER_TOTAL, D, HEAD_TOTAL * HEAD_DIM), D ** -0.5, 0.1875, ((0, 4), (2, 2))),
        "value_matrix": gaussian(splits[3], (LAYER_TOTAL, D, HEAD_TOTAL * HEAD_DIM), D ** -0.5, 0.1875, ((0, 4), (2, 2))),
        "output_gate_weight": gaussian(splits[4], (LAYER_TOTAL, D, HEAD_TOTAL * HEAD_DIM), D ** -0.5, 0.1875, ((0, 4), (2, 2))),
        "strength_weight": gaussian(splits[5], (LAYER_TOTAL, D, HEAD_TOTAL), D ** -0.5, 0.1875, ((0, 4), (2, 2))),
        "decay_input_weight": gaussian(splits[6], (LAYER_TOTAL, D, HEAD_TOTAL), D ** -0.5, 0.1875, ((0, 4), (2, 2))),
        "decay_scale_table": draw_decay_scale_table(jax.random.fold_in(splits[11], 71), part),
        "log_spike_decay": draw_log_spike_decay(jax.random.fold_in(splits[11], 71), part),
        "head_norm_gain": jnp.clip(1.0 + 0.18 * jax.random.normal(splits[9], (LAYER_TOTAL, HEAD_TOTAL * HEAD_DIM), jnp.float32), 0.1, 1.9),
        "closing_norm_gain": jnp.clip(1.0 + 0.18 * jax.random.normal(splits[10], (D,), jnp.float32), 0.1, 1.9),
    }


epsilon = 1e-06

def delta_rule(queries, keys_unit, values, beta_gate, decay_logarithm):
    length, head_count, head_width = queries.shape
    value_width = values.shape[-1]
    num_blocks = length // BLOCK
    best_precision = lax.Precision.HIGHEST

    def to_blocks(tensor):
        return tensor.reshape(num_blocks, BLOCK, head_count, -1).transpose(2, 0, 1, 3)
    query_b = to_blocks(queries)
    keys_b = to_blocks(keys_unit)
    values_b = to_blocks(values)
    beta_b = beta_gate.reshape(num_blocks, BLOCK, head_count).transpose(2, 0, 1)
    decay_b = decay_logarithm.reshape(num_blocks, BLOCK, head_count).transpose(2, 0, 1)
    cumulative = jnp.cumsum(decay_b, axis=-1)
    row_ids = lax.broadcasted_iota(jnp.int32, (BLOCK, BLOCK), 0)
    col_ids = lax.broadcasted_iota(jnp.int32, (BLOCK, BLOCK), 1)
    within = jnp.where(row_ids >= col_ids, cumulative[..., :, None] - cumulative[..., None, :], -jnp.inf)
    weights = jnp.exp(within)
    keys_beta = keys_b * beta_b[..., None]
    self_term = jnp.where(row_ids > col_ids, jnp.einsum('hnik,hnjk->hnij', keys_beta, keys_b, precision=best_precision) * weights, 0.0)
    system = self_term + jnp.eye(BLOCK, dtype=self_term.dtype)
    right_side = jnp.concatenate([values_b * beta_b[..., None], keys_beta * jnp.exp(cumulative)[..., None]], axis=-1)
    solved = jax.scipy.linalg.solve_triangular(system, right_side, lower=True, unit_diagonal=True)
    update = solved[..., :value_width]
    correct = solved[..., value_width:]
    scores = jnp.einsum('hnik,hnjk->hnij', query_b, keys_b, precision=best_precision) * weights
    query_dec = query_b * jnp.exp(cumulative)[..., None]
    keys_dec = keys_b * jnp.exp(cumulative[..., -1:] - cumulative)[..., None]
    block_decay = jnp.exp(cumulative[..., -1])

    def advance(state_matrix, inputs):
        state_update, correction_term, normed_queries, normed_keys, attention_scores, decay_factor = inputs
        new_state = state_update - jnp.einsum('rna,raq->rnq', correction_term, state_matrix, precision=best_precision)
        normed_output = jnp.einsum('rna,raq->rnq', normed_queries, state_matrix, precision=best_precision) + jnp.einsum('pak,pkr->par', attention_scores, new_state, precision=best_precision)
        state_matrix = state_matrix * decay_factor[:, None, None] + jnp.einsum('fni,fnl->fil', normed_keys, new_state, precision=best_precision)
        return (state_matrix, normed_output)
    sequence_in = tuple((jnp.moveaxis(tensor, 1, 0) for tensor in (update, correct, query_dec, keys_dec, scores, block_decay)))
    initial_state = jnp.zeros((head_count, head_width, value_width), jnp.float32)
    final_state, outputs = lax.scan(advance, initial_state, sequence_in)
    return outputs.transpose(0, 2, 1, 3).reshape(length, head_count, value_width)

def merge_head_outputs(query_projected, key_projected, value_projected, gate_logits, strength_logits, decay_logits, decay_speed, spike_log_values, gain_vector):
    length = query_projected.shape[0]
    head_count = strength_logits.shape[-1]
    head_width = query_projected.shape[1] // head_count

    def normalize(projected):
        activated = jax.nn.silu(projected).reshape(length, head_count, -1)
        return activated * lax.rsqrt(lax.optimization_barrier(jnp.sum(activated * activated, axis=-1, keepdims=True)) + epsilon)
    queries = normalize(query_projected) * head_width ** (-0.5)
    keys_unit = normalize(key_projected)
    values = jax.nn.silu(value_projected).reshape(length, head_count, -1)
    beta_gate = jax.nn.sigmoid(strength_logits)
    decay_logarithm = -decay_speed[None, :] * jax.nn.softplus(decay_logits) + spike_log_values
    mixed_out = delta_rule(queries, keys_unit, values, beta_gate, decay_logarithm)
    mixed_out = mixed_out * lax.rsqrt(lax.optimization_barrier(jnp.mean(mixed_out * mixed_out, axis=-1, keepdims=True)) + epsilon) * gain_vector.reshape(head_count, -1) * jax.nn.silu(gate_logits).reshape(length, head_count, -1)
    return mixed_out.reshape(length, -1).astype(jnp.bfloat16)

def reference(tokens, query_matrix, key_matrix, value_matrix, output_gate_weight, strength_weight, decay_input_weight, decay_scale_table, log_spike_decay, head_norm_gain, closing_norm_gain):
    hidden = tokens
    for layer_number in range(LAYER_TOTAL):
        flat_rows = hidden.reshape(-1, D)
        square = flat_rows.astype(jnp.float32)
        inv_rms = lax.rsqrt(lax.optimization_barrier(jnp.mean(square * square, axis=-1, keepdims=True)) + epsilon)
        projected = [(jnp.dot(flat_rows.astype(jnp.float32), matrix[layer_number].astype(jnp.float32), preferred_element_type=jnp.float32) * inv_rms).reshape(MICRO, SEQUENCE_LENGTH, -1) for matrix in (query_matrix, key_matrix, value_matrix, output_gate_weight, strength_weight, decay_input_weight)]
        token_mixer = partial(merge_head_outputs, decay_speed=decay_scale_table[layer_number], spike_log_values=log_spike_decay[layer_number], gain_vector=head_norm_gain[layer_number])
        mixed_out = jax.vmap(token_mixer)(projected[0], projected[1], projected[2], projected[3], projected[4], projected[5])
        hidden = (hidden.astype(jnp.float32) + mixed_out.astype(jnp.float32)).astype(jnp.bfloat16)
    square = hidden.astype(jnp.float32)
    inv_rms = lax.rsqrt(lax.optimization_barrier(jnp.mean(square * square, axis=-1, keepdims=True)) + epsilon)
    return (square * inv_rms * closing_norm_gain).astype(jnp.bfloat16)
```

```python
import functools
import jax
import jax.numpy as jnp
from jax import lax
from jax.experimental import pallas as pl
from jax.experimental.pallas import tpu as pltpu
from jax.sharding import PartitionSpec as P

epsilon = 1e-06
F32 = jnp.float32
BF16 = jnp.bfloat16
MESH = pl.DeviceIdType.MESH
NT = (((1,), (1,)), ((), ()))


def silu(a):
    return a / (1.0 + jnp.exp(-a))


def dot(a, b):
    return jnp.dot(a.astype(BF16), b.astype(BF16), preferred_element_type=F32)


def stack_kernel(
    stages,
    group,
    tokens,
    query_hbm,
    key_hbm,
    value_hbm,
    gate_hbm,
    strength,
    decay_in,
    decay_speed,
    spike,
    gain,
    closing_gain,
    out,
    weights,
    acc,
    xin,
    xout,
    yin,
    level,
    spike_columns,
    part_mine,
    part_other,
    w_sem,
    in_sem,
    entry_sem,
    fwd_send,
    fwd_recv,
    out_send,
    y_recv,
    part_send,
    part_recv,
):
    stage = lax.axis_index("pp")
    core = lax.axis_index("tp")
    last = stages - 1
    length, half = tokens.shape
    heads = xout.shape[1]
    width = half // heads
    model_width = group * half
    others = range(1, group)

    def peer(d):
        return lax.rem(core + d, group)

    loads = [
        pltpu.make_async_copy(ref, weights.at[i], w_sem.at[i])
        for i, ref in enumerate((query_hbm, key_hbm, value_hbm, gate_hbm))
    ]
    for load in loads:
        load.start()

    barrier = pltpu.get_barrier_semaphore()
    for d in range(1, stages):
        pl.semaphore_signal(
            barrier, inc=1, device_id={"pp": lax.rem(stage + d, stages)}, device_id_type=MESH
        )
    for d in others:
        pl.semaphore_signal(barrier, inc=1, device_id={"tp": peer(d)}, device_id_type=MESH)
    pl.semaphore_wait(barrier, stages + group - 2)

    def entry_copy(h):
        return pltpu.make_async_remote_copy(
            src_ref=xout.at[stages, h],
            dst_ref=xin.at[stage, core * heads + h],
            send_sem=entry_sem.at[h],
            recv_sem=in_sem.at[stage, h],
            device_id={"pp": 0},
            device_id_type=MESH,
        )

    def next_copy(m, h):
        return pltpu.make_async_remote_copy(
            src_ref=xout.at[m, h],
            dst_ref=xin.at[m, core * heads + h],
            send_sem=out_send.at[m, h],
            recv_sem=in_sem.at[m, h],
            device_id={"pp": lax.rem(stage + 1, stages)},
            device_id_type=MESH,
        )

    def exit_copy(m, h):
        return pltpu.make_async_remote_copy(
            src_ref=xout.at[m, h],
            dst_ref=yin.at[h],
            send_sem=out_send.at[m, h],
            recv_sem=y_recv.at[h],
            device_id={"pp": m},
            device_id_type=MESH,
        )

    def forward_copy(m, d, h):
        return pltpu.make_async_remote_copy(
            src_ref=xin.at[m, core * heads + h],
            dst_ref=xin.at[m, core * heads + h],
            send_sem=fwd_send.at[m, d - 1, h],
            recv_sem=fwd_recv.at[m, d - 1, h],
            device_id={"tp": peer(d)},
            device_id_type=MESH,
        )

    @pl.when(stage == 0)
    def _():
        for h in range(heads):
            xin[0, core * heads + h] = tokens[:, h * width : (h + 1) * width]

    @pl.when(stage > 0)
    def _():
        for h in range(heads):
            xout[stages, h] = tokens[:, h * width : (h + 1) * width]
        for h in range(heads):
            entry_copy(h).start()

    rows = lax.broadcasted_iota(jnp.int32, (length, length), 0)
    cols = lax.broadcasted_iota(jnp.int32, (length, length), 1)
    differ = rows ^ cols
    found = jnp.full((length, length), -1, jnp.int32)
    level_count = (length - 1).bit_length()
    for k in range(level_count):
        found = found + (differ >= (1 << k)).astype(jnp.int32)
    level[...] = jnp.where(rows > cols, found, jnp.where(rows == cols, -1, -2))

    spike_columns[...] = jnp.concatenate(
        [spike[...], jnp.zeros((length - heads, length), F32)], axis=0
    ).T

    def step(m, _):
        @pl.when((stage > 0) | (m > 0))
        def _():
            for h in range(heads):
                next_copy(m, h).wait_recv()
                for d in others:
                    forward_copy(m, d, h).start()

        @pl.when((stage == 0) & (m == 0))
        def _():
            for h in range(heads):
                for d in others:
                    forward_copy(m, d, h).start()

        @pl.when(m == 0)
        def _():
            for load in loads:
                load.wait()

        def gather(which):
            return jnp.concatenate([xin[m, which * heads + h] for h in range(heads)], axis=1)

        def project(x, which):
            own = pl.ds(pl.multiple_of(which * half, half), half)
            mats = [dot(x, weights[i, own, :]) for i in range(4)]
            small = [
                lax.dot_general(x, ref[:, own], NT, preferred_element_type=F32)
                for ref in (strength, decay_in)
            ]
            wide = x.astype(F32)
            return mats, small, jnp.sum(wide * wide, axis=1, keepdims=True)

        mats, small, squares = project(gather(core), core)
        for i in range(4):
            acc[i] = mats[i]
        for d in others:
            for h in range(heads):
                forward_copy(m, d, h).wait_recv()
            source = peer(group - d)
            mats, small_other, squares_other = project(gather(source), source)
            small = [a + b for a, b in zip(small, small_other)]
            squares = squares + squares_other
            if d < group - 1:
                for i in range(4):
                    acc[i] += mats[i]
        inv_rms = lax.rsqrt(squares / model_width + epsilon)
        beta = 1.0 / (1.0 + jnp.exp(-small[0] * inv_rms))
        pre = small[1][:, :heads] * inv_rms
        softplus = jnp.maximum(pre, 0.0) + jnp.log(1.0 + jnp.exp(-jnp.abs(pre)))
        log_decay = -decay_speed[...] * softplus + spike_columns[:, :heads]
        lev = level[...]
        lower = jnp.where(lev >= -1, 1.0, 0.0).astype(F32)
        padded = jnp.concatenate(
            [log_decay, jnp.zeros((length, length - heads), F32)], axis=1
        )
        cumulative = jnp.dot(
            lower, padded, precision=lax.Precision.HIGHEST, preferred_element_type=F32
        )
        cumulative_rows = cumulative.T
        every = range(heads)

        def columns(i, h):
            part = slice(h * width, (h + 1) * width)
            return (acc[i, :, part] + mats[i][:, part]) * inv_rms

        def unit(a):
            return a * lax.rsqrt(jnp.sum(a * a, axis=1, keepdims=True) + epsilon)

        keys = [unit(silu(columns(1, h))) for h in every]
        queries = [unit(silu(columns(0, h))) * width ** (-0.5) for h in every]
        gram = []
        for h in every:
            left = jnp.concatenate([keys[h] * beta[:, h : h + 1], queries[h]], axis=0)
            gram.append(
                lax.dot_general(
                    left.astype(BF16), keys[h].astype(BF16), NT, preferred_element_type=F32
                )
            )
        decayed = [
            jnp.exp(
                jnp.where(
                    lev >= -1, cumulative[:, h : h + 1] - cumulative_rows[h : h + 1, :], -jnp.inf
                )
            )
            for h in every
        ]
        system = [gram[h][:length] * decayed[h] for h in every]
        scores = [(gram[h][length:] * decayed[h]).astype(BF16) for h in every]

        def corner(h, k):
            return jnp.where(lev == k, system[h], 0.0).astype(BF16)

        eye = jnp.where(lev == -1, 1.0, 0.0).astype(F32)
        inverse = [eye - jnp.where(lev == 0, system[h], 0.0) for h in every]
        for k in range(1, level_count - 1):
            rounded = [inverse[h].astype(BF16) for h in every]
            partial = [dot(corner(h, k), rounded[h]) for h in every]
            inverse = [inverse[h] - dot(rounded[h], partial[h]) for h in every]
        rounded = [inverse[h].astype(BF16) for h in every]
        values = [silu(columns(2, h)) * beta[:, h : h + 1] for h in every]
        first = [dot(rounded[h], values[h]) for h in every]
        partial = [dot(corner(h, level_count - 1), first[h]) for h in every]
        update = [first[h] - dot(rounded[h], partial[h]) for h in every]
        mixed = [dot(scores[h], update[h]) for h in every]
        for h in every:
            gate = silu(columns(3, h))
            scale = lax.rsqrt(jnp.mean(mixed[h] * mixed[h], axis=1, keepdims=True) + epsilon)
            head_out = mixed[h] * scale * gain[:, h * width : (h + 1) * width] * gate
            before = xin[m, core * heads + h].astype(F32)
            xout[m, h] = (before + head_out.astype(BF16).astype(F32)).astype(BF16)

        @pl.when(stage < last)
        def _():
            for h in range(heads):
                next_copy(m, h).start()

        @pl.when((stage == last) & (m < last))
        def _():
            for h in range(heads):
                exit_copy(m, h).start()

        return 0

    lax.fori_loop(0, stages, step, 0)

    @pl.when(stage == last)
    def _():
        for h in range(heads):
            yin[h] = xout[last, h]

    @pl.when(stage < last)
    def _():
        for h in range(heads):
            exit_copy(0, h).wait_recv()

    final = [yin[h].astype(F32) for h in range(heads)]
    total = sum(jnp.sum(a * a, axis=1, keepdims=True) for a in final)
    part_mine[...] = jnp.broadcast_to(total, part_mine.shape)
    part_copies = [
        pltpu.make_async_remote_copy(
            src_ref=part_mine,
            dst_ref=part_other.at[d - 1],
            send_sem=part_send.at[d - 1],
            recv_sem=part_recv.at[d - 1],
            device_id={"tp": peer(d)},
            device_id_type=MESH,
        )
        for d in others
    ]
    for copy in part_copies:
        copy.start()

    @pl.when(stage > 0)
    def _():
        for h in range(heads):
            entry_copy(h).wait_send()

    def drain(m, _):
        for h in range(heads):
            for d in others:
                forward_copy(m, d, h).wait_send()

        @pl.when((stage < last) | (m < last))
        def _():
            for h in range(heads):
                next_copy(m, h).wait_send()

        return 0

    lax.fori_loop(0, stages, drain, 0)
    total = part_mine[...]
    for copy in part_copies:
        copy.wait()
    for d in others:
        total = total + part_other[d - 1]
    inv_rms = lax.rsqrt(total / model_width + epsilon)
    for h in range(heads):
        part = slice(h * width, (h + 1) * width)
        out[:, part] = (final[h] * inv_rms * closing_gain[:, part]).astype(BF16)


def on_device(
    stages,
    group,
    tokens,
    query_matrix,
    key_matrix,
    value_matrix,
    output_gate_weight,
    strength_weight,
    decay_input_weight,
    decay_scale_table,
    log_spike_decay,
    head_norm_gain,
    closing_norm_gain,
):
    _, length, half = tokens.shape
    heads = strength_weight.shape[-1]
    width = half // heads

    def rows_of(weight):
        return jnp.pad(weight[0].T, ((0, 1), (0, 0))) if heads == 1 else weight[0].T

    vmem = pl.BlockSpec(memory_space=pltpu.VMEM)
    anywhere = pl.BlockSpec(memory_space=pl.ANY)
    dma = pltpu.SemaphoreType.DMA
    result = pl.pallas_call(
        functools.partial(stack_kernel, stages, group),
        out_shape=jax.ShapeDtypeStruct((length, half), BF16),
        in_specs=[vmem] + [anywhere] * 4 + [vmem] * 6,
        out_specs=vmem,
        scratch_shapes=[
            pltpu.VMEM((4, group * half, half), BF16),
            pltpu.VMEM((4, length, half), F32),
            pltpu.VMEM((stages, group * heads, length, width), BF16),
            pltpu.VMEM((stages + 1, heads, length, width), BF16),
            pltpu.VMEM((heads, length, width), BF16),
            pltpu.VMEM((length, length), jnp.int32),
            pltpu.VMEM((length, length), F32),
            pltpu.VMEM((length, width), F32),
            pltpu.VMEM((group - 1, length, width), F32),
            dma((4,)),
            dma((stages, heads)),
            dma((heads,)),
            dma((stages, group - 1, heads)),
            dma((stages, group - 1, heads)),
            dma((stages, heads)),
            dma((heads,)),
            dma((group - 1,)),
            dma((group - 1,)),
        ],
        compiler_params=pltpu.CompilerParams(
            collective_id=0, has_side_effects=True, vmem_limit_bytes=60 * 1024 * 1024
        ),
    )(
        tokens[0],
        query_matrix[0],
        key_matrix[0],
        value_matrix[0],
        output_gate_weight[0],
        rows_of(strength_weight),
        rows_of(decay_input_weight),
        decay_scale_table,
        log_spike_decay[0].T,
        head_norm_gain,
        closing_norm_gain[None],
    )
    return result[None]


def solution(mesh):
    placed = (
        P("pp", "fs", "tp"),
        P("pp", None, "tp"),
        P("pp", None, "tp"),
        P("pp", None, "tp"),
        P("pp", None, "tp"),
        P("pp", None, "tp"),
        P("pp", None, "tp"),
        P("pp", "tp"),
        P("pp", None, "tp"),
        P("pp", "tp"),
        P("tp"),
    )
    return jax.shard_map(
        functools.partial(on_device, mesh.shape["pp"], mesh.shape["tp"]),
        mesh=mesh,
        in_specs=placed,
        out_specs=P("pp", "fs", "tp"),
        check_vma=False,
    )
```

```python
import functools
import jax
import jax.numpy as jnp
from jax import lax
from jax.experimental import pallas as pl
from jax.experimental.pallas import tpu as pltpu
from jax.sharding import PartitionSpec as P

epsilon = 1e-06
F32 = jnp.float32
BF16 = jnp.bfloat16
MESH = pl.DeviceIdType.MESH
NT = (((1,), (1,)), ((), ()))


def silu(a):
    return a / (1.0 + jnp.exp(-a))


def dot(a, b):
    return jnp.dot(a.astype(BF16), b.astype(BF16), preferred_element_type=F32)


def stack_kernel(
    stages,
    group,
    tokens,
    query_hbm,
    key_hbm,
    value_hbm,
    gate_hbm,
    strength_hbm,
    decay_in_hbm,
    decay_speed_hbm,
    spike_hbm,
    gain_hbm,
    closing_hbm,
    out,
    strength,
    decay_in,
    decay_speed,
    spike,
    gain,
    closing_gain,
    weights,
    acc,
    xin,
    xout,
    yin,
    level,
    spike_columns,
    part_mine,
    part_other,
    w_sem,
    small_sem,
    token_sem,
    go_sem,
    in_sem,
    entry_sem,
    fwd_send,
    fwd_recv,
    out_send,
    y_recv,
    part_send,
    part_recv,
):
    stage = lax.axis_index("pp")
    core = lax.axis_index("tp")
    last = stages - 1
    length, half = tokens.shape
    heads = xout.shape[1]
    width = half // heads
    model_width = group * half
    others = range(1, group)

    def peer(d):
        return lax.rem(core + d, group)

    barrier = pltpu.get_barrier_semaphore()
    for d in range(1, stages):
        pl.semaphore_signal(
            barrier, inc=1, device_id={"pp": lax.rem(stage + d, stages)}, device_id_type=MESH
        )
    for d in others:
        pl.semaphore_signal(barrier, inc=1, device_id={"tp": peer(d)}, device_id_type=MESH)

    def token_copy(h, target):
        return pltpu.make_async_copy(
            tokens.at[:, h * width : (h + 1) * width], target, token_sem.at[h]
        )

    @pl.when(stage == 0)
    def _():
        for h in range(heads):
            token_copy(h, xin.at[0, core * heads + h]).start()

    @pl.when(stage > 0)
    def _():
        for h in range(heads):
            token_copy(h, xout.at[stages, h]).start()

    small_loads = [
        pltpu.make_async_copy(a, b, small_sem.at[i])
        for i, (a, b) in enumerate(
            (
                (strength_hbm, strength),
                (decay_in_hbm, decay_in),
                (decay_speed_hbm, decay_speed),
                (spike_hbm, spike),
                (gain_hbm, gain),
                (closing_hbm, closing_gain),
            )
        )
    ]
    for load in small_loads:
        load.start()
    loads = [
        pltpu.make_async_copy(ref, weights.at[i], w_sem.at[i])
        for i, ref in enumerate((query_hbm, key_hbm, value_hbm, gate_hbm))
    ]
    for load in loads:
        load.start()

    pl.semaphore_wait(barrier, stages + group - 2)

    def entry_copy(h):
        return pltpu.make_async_remote_copy(
            src_ref=xout.at[stages, h],
            dst_ref=xin.at[stage, core * heads + h],
            send_sem=entry_sem.at[h],
            recv_sem=in_sem.at[stage, h],
            device_id={"pp": 0},
            device_id_type=MESH,
        )

    def next_copy(m, h):
        return pltpu.make_async_remote_copy(
            src_ref=xout.at[m, h],
            dst_ref=xin.at[m, core * heads + h],
            send_sem=out_send.at[m, h],
            recv_sem=in_sem.at[m, h],
            device_id={"pp": lax.rem(stage + 1, stages)},
            device_id_type=MESH,
        )

    def exit_copy(m, h):
        return pltpu.make_async_remote_copy(
            src_ref=xout.at[m, h],
            dst_ref=yin.at[h],
            send_sem=out_send.at[m, h],
            recv_sem=y_recv.at[h],
            device_id={"pp": m},
            device_id_type=MESH,
        )

    def forward_copy(m, d, h):
        return pltpu.make_async_remote_copy(
            src_ref=xin.at[m, core * heads + h],
            dst_ref=xin.at[m, core * heads + h],
            send_sem=fwd_send.at[m, d - 1, h],
            recv_sem=fwd_recv.at[m, d - 1, h],
            device_id={"tp": peer(d)},
            device_id_type=MESH,
        )

    @pl.when(stage == 0)
    def _():
        for h in range(heads):
            token_copy(h, xin.at[0, core * heads + h]).wait()

    early = max(heads - 2, 0)

    @pl.when(stage > 0)
    def _():
        for h in range(heads):
            token_copy(h, xout.at[stages, h]).wait()

        @pl.when(stage > 1)
        def _():
            pl.semaphore_wait(go_sem, 1)

        for h in range(heads):
            entry_copy(h).start()
        entry_copy(early).wait_send()

        @pl.when(stage < last)
        def _():
            pl.semaphore_signal(
                go_sem, inc=1, device_id={"pp": lax.rem(stage + 1, stages)}, device_id_type=MESH
            )

    rows = lax.broadcasted_iota(jnp.int32, (length, length), 0)
    cols = lax.broadcasted_iota(jnp.int32, (length, length), 1)
    differ = rows ^ cols
    found = jnp.full((length, length), -1, jnp.int32)
    level_count = (length - 1).bit_length()
    for k in range(level_count):
        found = found + (differ >= (1 << k)).astype(jnp.int32)
    level[...] = jnp.where(rows > cols, found, jnp.where(rows == cols, -1, -2))

    for load in small_loads:
        load.wait()
    spike_columns[...] = jnp.concatenate(
        [spike[...], jnp.zeros((length - heads, length), F32)], axis=0
    ).T

    def step(m, _):
        @pl.when((stage > 0) | (m > 0))
        def _():
            for h in range(heads):
                next_copy(m, h).wait_recv()
                for d in others:
                    forward_copy(m, d, h).start()

        @pl.when((stage == 0) & (m == 0))
        def _():
            for h in range(heads):
                for d in others:
                    forward_copy(m, d, h).start()

        @pl.when(m == 0)
        def _():
            for load in loads:
                load.wait()

        def gather(which):
            return jnp.concatenate([xin[m, which * heads + h] for h in range(heads)], axis=1)

        def project(x, which):
            own = pl.ds(pl.multiple_of(which * half, half), half)
            mats = [dot(x, weights[i, own, :]) for i in range(4)]
            small = [
                lax.dot_general(x, ref[:, own], NT, preferred_element_type=F32)
                for ref in (strength, decay_in)
            ]
            wide = x.astype(F32)
            return mats, small, jnp.sum(wide * wide, axis=1, keepdims=True)

        mats, small, squares = project(gather(core), core)
        for i in range(4):
            acc[i] = mats[i]
        for d in others:
            for h in range(heads):
                forward_copy(m, d, h).wait_recv()
            source = peer(group - d)
            mats, small_other, squares_other = project(gather(source), source)
            small = [a + b for a, b in zip(small, small_other)]
            squares = squares + squares_other
            if d < group - 1:
                for i in range(4):
                    acc[i] += mats[i]
        inv_rms = lax.rsqrt(squares / model_width + epsilon)
        beta = 1.0 / (1.0 + jnp.exp(-small[0] * inv_rms))
        pre = small[1][:, :heads] * inv_rms
        softplus = jnp.maximum(pre, 0.0) + jnp.log(1.0 + jnp.exp(-jnp.abs(pre)))
        log_decay = -decay_speed[...] * softplus + spike_columns[:, :heads]
        lev = level[...]
        lower = jnp.where(lev >= -1, 1.0, 0.0).astype(F32)
        padded = jnp.concatenate(
            [log_decay, jnp.zeros((length, length - heads), F32)], axis=1
        )
        cumulative = jnp.dot(
            lower, padded, precision=lax.Precision.HIGHEST, preferred_element_type=F32
        )
        cumulative_rows = cumulative.T
        every = range(heads)

        def columns(i, h):
            part = slice(h * width, (h + 1) * width)
            return (acc[i, :, part] + mats[i][:, part]) * inv_rms

        def unit(a):
            return a * lax.rsqrt(jnp.sum(a * a, axis=1, keepdims=True) + epsilon)

        keys = [unit(silu(columns(1, h))) for h in every]
        queries = [unit(silu(columns(0, h))) * width ** (-0.5) for h in every]
        gram = []
        for h in every:
            left = jnp.concatenate([keys[h] * beta[:, h : h + 1], queries[h]], axis=0)
            gram.append(
                lax.dot_general(
                    left.astype(BF16), keys[h].astype(BF16), NT, preferred_element_type=F32
                )
            )
        decayed = [
            jnp.exp(
                jnp.where(
                    lev >= -1, cumulative[:, h : h + 1] - cumulative_rows[h : h + 1, :], -jnp.inf
                )
            )
            for h in every
        ]
        system = [gram[h][:length] * decayed[h] for h in every]
        scores = [(gram[h][length:] * decayed[h]).astype(BF16) for h in every]

        def corner(h, k):
            return jnp.where(lev == k, system[h], 0.0).astype(BF16)

        eye = jnp.where(lev == -1, 1.0, 0.0).astype(F32)
        inverse = [eye - jnp.where(lev == 0, system[h], 0.0) for h in every]
        for k in range(1, level_count - 1):
            rounded = [inverse[h].astype(BF16) for h in every]
            partial = [dot(corner(h, k), rounded[h]) for h in every]
            inverse = [inverse[h] - dot(rounded[h], partial[h]) for h in every]
        rounded = [inverse[h].astype(BF16) for h in every]
        values = [silu(columns(2, h)) * beta[:, h : h + 1] for h in every]
        first = [dot(rounded[h], values[h]) for h in every]
        partial = [dot(corner(h, level_count - 1), first[h]) for h in every]
        update = [first[h] - dot(rounded[h], partial[h]) for h in every]
        mixed = [dot(scores[h], update[h]) for h in every]
        for h in every:
            gate = silu(columns(3, h))
            scale = lax.rsqrt(jnp.mean(mixed[h] * mixed[h], axis=1, keepdims=True) + epsilon)
            head_out = mixed[h] * scale * gain[:, h * width : (h + 1) * width] * gate
            before = xin[m, core * heads + h].astype(F32)
            xout[m, h] = (before + head_out.astype(BF16).astype(F32)).astype(BF16)

        @pl.when(stage < last)
        def _():
            for h in range(heads):
                next_copy(m, h).start()

        @pl.when((stage == last) & (m < last))
        def _():
            for h in range(heads):
                exit_copy(m, h).start()

        return 0

    lax.fori_loop(0, stages, step, 0)

    @pl.when(stage == last)
    def _():
        for h in range(heads):
            yin[h] = xout[last, h]

    @pl.when(stage < last)
    def _():
        for h in range(heads):
            exit_copy(0, h).wait_recv()

    final = [yin[h].astype(F32) for h in range(heads)]
    total = sum(jnp.sum(a * a, axis=1, keepdims=True) for a in final)
    part_mine[...] = jnp.broadcast_to(total, part_mine.shape)
    part_copies = [
        pltpu.make_async_remote_copy(
            src_ref=part_mine,
            dst_ref=part_other.at[d - 1],
            send_sem=part_send.at[d - 1],
            recv_sem=part_recv.at[d - 1],
            device_id={"tp": peer(d)},
            device_id_type=MESH,
        )
        for d in others
    ]
    for copy in part_copies:
        copy.start()

    @pl.when(stage > 0)
    def _():
        for h in range(heads):
            if h != early:
                entry_copy(h).wait_send()

    def drain(m, _):
        for h in range(heads):
            for d in others:
                forward_copy(m, d, h).wait_send()

        @pl.when((stage < last) | (m < last))
        def _():
            for h in range(heads):
                next_copy(m, h).wait_send()

        return 0

    lax.fori_loop(0, stages, drain, 0)
    total = part_mine[...]
    for copy in part_copies:
        copy.wait()
    for d in others:
        total = total + part_other[d - 1]
    inv_rms = lax.rsqrt(total / model_width + epsilon)
    for h in range(heads):
        part = slice(h * width, (h + 1) * width)
        out[:, part] = (final[h] * inv_rms * closing_gain[:, part]).astype(BF16)


def on_device(
    stages,
    group,
    tokens,
    query_matrix,
    key_matrix,
    value_matrix,
    output_gate_weight,
    strength_weight,
    decay_input_weight,
    decay_scale_table,
    log_spike_decay,
    head_norm_gain,
    closing_norm_gain,
):
    _, length, half = tokens.shape
    heads = strength_weight.shape[-1]
    width = half // heads

    def rows_of(weight):
        return jnp.pad(weight[0].T, ((0, 1), (0, 0))) if heads == 1 else weight[0].T

    vmem = pl.BlockSpec(memory_space=pltpu.VMEM)
    anywhere = pl.BlockSpec(memory_space=pltpu.HBM)
    dma = pltpu.SemaphoreType.DMA
    result = pl.pallas_call(
        functools.partial(stack_kernel, stages, group),
        out_shape=pltpu.VMEM((length, half), BF16),
        in_specs=[anywhere] * 11,
        out_specs=vmem,
        scratch_shapes=[
            pltpu.VMEM((max(heads, 2), group * half), BF16),
            pltpu.VMEM((max(heads, 2), group * half), BF16),
            pltpu.VMEM((1, heads), F32),
            pltpu.VMEM((heads, length), F32),
            pltpu.VMEM((1, half), F32),
            pltpu.VMEM((1, half), F32),
            pltpu.VMEM((4, group * half, half), BF16),
            pltpu.VMEM((4, length, half), F32),
            pltpu.VMEM((stages, group * heads, length, width), BF16),
            pltpu.VMEM((stages + 1, heads, length, width), BF16),
            pltpu.VMEM((heads, length, width), BF16),
            pltpu.VMEM((length, length), jnp.int32),
            pltpu.VMEM((length, length), F32),
            pltpu.VMEM((length, width), F32),
            pltpu.VMEM((group - 1, length, width), F32),
            dma((4,)),
            dma((6,)),
            dma((heads,)),
            pltpu.SemaphoreType.REGULAR,
            dma((stages, heads)),
            dma((heads,)),
            dma((stages, group - 1, heads)),
            dma((stages, group - 1, heads)),
            dma((stages, heads)),
            dma((heads,)),
            dma((group - 1,)),
            dma((group - 1,)),
        ],
        compiler_params=pltpu.CompilerParams(
            collective_id=0, has_side_effects=True, vmem_limit_bytes=60 * 1024 * 1024
        ),
    )(
        tokens[0],
        query_matrix[0],
        key_matrix[0],
        value_matrix[0],
        output_gate_weight[0],
        rows_of(strength_weight),
        rows_of(decay_input_weight),
        decay_scale_table,
        log_spike_decay[0].T,
        head_norm_gain,
        closing_norm_gain[None],
    )
    return result[None]


def solution(mesh):
    placed = (
        P("pp", "fs", "tp"),
        P("pp", None, "tp"),
        P("pp", None, "tp"),
        P("pp", None, "tp"),
        P("pp", None, "tp"),
        P("pp", None, "tp"),
        P("pp", None, "tp"),
        P("pp", "tp"),
        P("pp", None, "tp"),
        P("pp", "tp"),
        P("tp"),
    )
    return jax.shard_map(
        functools.partial(on_device, mesh.shape["pp"], mesh.shape["tp"]),
        mesh=mesh,
        in_specs=placed,
        out_specs=P("pp", "fs", "tp"),
        check_vma=False,
    )
```

```python
import functools
import jax
import jax.numpy as jnp
from jax import lax
from jax.experimental import pallas as pl
from jax.experimental.pallas import tpu as pltpu
from jax.sharding import PartitionSpec as P

epsilon = 1e-06
F32 = jnp.float32
BF16 = jnp.bfloat16
MESH = pl.DeviceIdType.MESH
NT = (((1,), (1,)), ((), ()))


def silu(a):
    return a / (1.0 + jnp.exp(-a))


def dot(a, b):
    return jnp.dot(a.astype(BF16), b.astype(BF16), preferred_element_type=F32)


def stack_kernel(
    stages,
    group,
    tokens,
    query_hbm,
    key_hbm,
    value_hbm,
    gate_hbm,
    strength_hbm,
    decay_in_hbm,
    decay_speed_hbm,
    spike_hbm,
    gain_hbm,
    closing_hbm,
    out,
    strength,
    decay_in,
    decay_speed,
    spike,
    gain,
    closing_gain,
    weights,
    acc,
    xin,
    xout,
    yin,
    level,
    spike_columns,
    part_mine,
    part_other,
    w_sem,
    small_sem,
    token_sem,
    go_sem,
    in_sem,
    entry_sem,
    fwd_send,
    fwd_recv,
    out_send,
    y_recv,
    part_send,
    part_recv,
):
    stage = lax.axis_index("pp")
    core = lax.axis_index("tp")
    last = stages - 1
    length, half = tokens.shape
    heads = xout.shape[1]
    width = half // heads
    model_width = group * half
    others = range(1, group)

    def peer(d):
        return lax.rem(core + d, group)

    barrier = pltpu.get_barrier_semaphore()
    for d in range(1, stages):
        pl.semaphore_signal(
            barrier, inc=1, device_id={"pp": lax.rem(stage + d, stages)}, device_id_type=MESH
        )
    for d in others:
        pl.semaphore_signal(barrier, inc=1, device_id={"tp": peer(d)}, device_id_type=MESH)

    def token_copy(h, target):
        return pltpu.make_async_copy(
            tokens.at[:, h * width : (h + 1) * width], target, token_sem.at[h]
        )

    @pl.when(stage == 0)
    def _():
        for h in range(heads):
            token_copy(h, xin.at[0, core * heads + h]).start()

    @pl.when(stage > 0)
    def _():
        for h in range(heads):
            token_copy(h, xout.at[stages, h]).start()

    small_loads = [
        pltpu.make_async_copy(a, b, small_sem.at[i])
        for i, (a, b) in enumerate(
            (
                (strength_hbm, strength),
                (decay_in_hbm, decay_in),
                (decay_speed_hbm, decay_speed),
                (spike_hbm, spike),
                (gain_hbm, gain),
                (closing_hbm, closing_gain),
            )
        )
    ]
    for load in small_loads:
        load.start()
    loads = [
        pltpu.make_async_copy(ref, weights.at[i], w_sem.at[i])
        for i, ref in enumerate((query_hbm, key_hbm, value_hbm, gate_hbm))
    ]
    for load in loads:
        load.start()

    pl.semaphore_wait(barrier, stages + group - 2)

    def entry_copy(h):
        return pltpu.make_async_remote_copy(
            src_ref=xout.at[stages, h],
            dst_ref=xin.at[stage, core * heads + h],
            send_sem=entry_sem.at[h],
            recv_sem=in_sem.at[stage, h],
            device_id={"pp": 0},
            device_id_type=MESH,
        )

    def next_copy(m, h):
        return pltpu.make_async_remote_copy(
            src_ref=xout.at[m, h],
            dst_ref=xin.at[m, core * heads + h],
            send_sem=out_send.at[m, h],
            recv_sem=in_sem.at[m, h],
            device_id={"pp": lax.rem(stage + 1, stages)},
            device_id_type=MESH,
        )

    def exit_copy(m, h):
        return pltpu.make_async_remote_copy(
            src_ref=xout.at[m, h],
            dst_ref=yin.at[h],
            send_sem=out_send.at[m, h],
            recv_sem=y_recv.at[h],
            device_id={"pp": m},
            device_id_type=MESH,
        )

    def forward_copy(m, d, h):
        return pltpu.make_async_remote_copy(
            src_ref=xin.at[m, core * heads + h],
            dst_ref=xin.at[m, core * heads + h],
            send_sem=fwd_send.at[m, d - 1, h],
            recv_sem=fwd_recv.at[m, d - 1, h],
            device_id={"tp": peer(d)},
            device_id_type=MESH,
        )

    @pl.when(stage == 0)
    def _():
        for h in range(heads):
            token_copy(h, xin.at[0, core * heads + h]).wait()

    early = max(heads - 2, 0)

    @pl.when(stage > 0)
    def _():
        for h in range(heads):
            token_copy(h, xout.at[stages, h]).wait()

        @pl.when(stage > 1)
        def _():
            pl.semaphore_wait(go_sem, 1)

        for h in range(heads):
            entry_copy(h).start()
        entry_copy(early).wait_send()

        @pl.when(stage < last)
        def _():
            pl.semaphore_signal(
                go_sem, inc=1, device_id={"pp": lax.rem(stage + 1, stages)}, device_id_type=MESH
            )

    rows = lax.broadcasted_iota(jnp.int32, (length, length), 0)
    cols = lax.broadcasted_iota(jnp.int32, (length, length), 1)
    differ = rows ^ cols
    found = jnp.full((length, length), -1, jnp.int32)
    level_count = (length - 1).bit_length()
    for k in range(level_count):
        found = found + (differ >= (1 << k)).astype(jnp.int32)
    level[...] = jnp.where(rows > cols, found, jnp.where(rows == cols, -1, -2))

    for load in small_loads:
        load.wait()
    spike_columns[...] = jnp.concatenate(
        [spike[...], jnp.zeros((length - heads, length), F32)], axis=0
    ).T

    def finish(m, every, part, source, inv_rms, beta, cumulative, cumulative_rows):
        own = pl.ds(pl.multiple_of(source * half, half), half)
        wanted = slice(every[0] * width, (every[-1] + 1) * width)
        mats = [dot(part, weights[i, own, wanted]) for i in range(4)]
        lev = level[...]

        def columns(i, h):
            at = (h - every[0]) * width
            before = acc[i, :, h * width : (h + 1) * width]
            return (before + mats[i][:, at : at + width]) * inv_rms

        def unit(a):
            return a * lax.rsqrt(jnp.sum(a * a, axis=1, keepdims=True) + epsilon)

        keys = {h: unit(silu(columns(1, h))) for h in every}
        queries = {h: unit(silu(columns(0, h))) * width ** (-0.5) for h in every}
        gram = {}
        for h in every:
            left = jnp.concatenate([keys[h] * beta[:, h : h + 1], queries[h]], axis=0)
            gram[h] = lax.dot_general(
                left.astype(BF16), keys[h].astype(BF16), NT, preferred_element_type=F32
            )
        decayed = {
            h: jnp.exp(
                jnp.where(
                    lev >= -1, cumulative[:, h : h + 1] - cumulative_rows[h : h + 1, :], -jnp.inf
                )
            )
            for h in every
        }
        system = {h: gram[h][:length] * decayed[h] for h in every}
        scores = {h: (gram[h][length:] * decayed[h]).astype(BF16) for h in every}

        def corner(h, k):
            return jnp.where(lev == k, system[h], 0.0).astype(BF16)

        eye = jnp.where(lev == -1, 1.0, 0.0).astype(F32)
        inverse = {h: eye - jnp.where(lev == 0, system[h], 0.0) for h in every}
        for k in range(1, level_count - 1):
            rounded = {h: inverse[h].astype(BF16) for h in every}
            partial = {h: dot(corner(h, k), rounded[h]) for h in every}
            inverse = {h: inverse[h] - dot(rounded[h], partial[h]) for h in every}
        rounded = {h: inverse[h].astype(BF16) for h in every}
        values = {h: silu(columns(2, h)) * beta[:, h : h + 1] for h in every}
        first = {h: dot(rounded[h], values[h]) for h in every}
        partial = {h: dot(corner(h, level_count - 1), first[h]) for h in every}
        update = {h: first[h] - dot(rounded[h], partial[h]) for h in every}
        mixed = {h: dot(scores[h], update[h]) for h in every}
        for h in every:
            gate = silu(columns(3, h))
            scale = lax.rsqrt(jnp.mean(mixed[h] * mixed[h], axis=1, keepdims=True) + epsilon)
            head_out = mixed[h] * scale * gain[:, h * width : (h + 1) * width] * gate
            before = xin[m, core * heads + h].astype(F32)
            xout[m, h] = (before + head_out.astype(BF16).astype(F32)).astype(BF16)

        @pl.when(stage < last)
        def _():
            for h in every:
                next_copy(m, h).start()

        @pl.when((stage == last) & (m < last))
        def _():
            for h in every:
                exit_copy(m, h).start()

    def step(m, _):
        @pl.when((stage > 0) | (m > 0))
        def _():
            for h in range(heads):
                next_copy(m, h).wait_recv()
                for d in others:
                    forward_copy(m, d, h).start()

        @pl.when((stage == 0) & (m == 0))
        def _():
            for h in range(heads):
                for d in others:
                    forward_copy(m, d, h).start()

        @pl.when(m == 0)
        def _():
            for load in loads:
                load.wait()

        def gather(which):
            return jnp.concatenate([xin[m, which * heads + h] for h in range(heads)], axis=1)

        def rows_from(which):
            return pl.ds(pl.multiple_of(which * half, half), half)

        def project(x, which):
            small = [
                lax.dot_general(x, ref[:, rows_from(which)], NT, preferred_element_type=F32)
                for ref in (strength, decay_in)
            ]
            wide = x.astype(F32)
            return small, jnp.sum(wide * wide, axis=1, keepdims=True)

        own_part = gather(core)
        small, squares = project(own_part, core)
        for i in range(4):
            acc[i] = dot(own_part, weights[i, rows_from(core), :])
        for d in others:
            for h in range(heads):
                forward_copy(m, d, h).wait_recv()
            source = peer(group - d)
            part = gather(source)
            small_other, squares_other = project(part, source)
            small = [a + b for a, b in zip(small, small_other)]
            squares = squares + squares_other
            if d < group - 1:
                for i in range(4):
                    acc[i] += dot(part, weights[i, rows_from(source), :])
        inv_rms = lax.rsqrt(squares / model_width + epsilon)
        beta = 1.0 / (1.0 + jnp.exp(-small[0] * inv_rms))
        pre = small[1][:, :heads] * inv_rms
        softplus = jnp.maximum(pre, 0.0) + jnp.log(1.0 + jnp.exp(-jnp.abs(pre)))
        log_decay = -decay_speed[...] * softplus + spike_columns[:, :heads]
        lev = level[...]
        lower = jnp.where(lev >= -1, 1.0, 0.0).astype(F32)
        padded = jnp.concatenate(
            [log_decay, jnp.zeros((length, length - heads), F32)], axis=1
        )
        cumulative = jnp.dot(
            lower, padded, precision=lax.Precision.HIGHEST, preferred_element_type=F32
        )
        cumulative_rows = cumulative.T
        pair = max(heads // 2, 1)
        for every in [range(a, a + pair) for a in range(0, heads, pair)]:
            finish(m, every, part, source, inv_rms, beta, cumulative, cumulative_rows)


        return 0

    lax.fori_loop(0, stages, step, 0)

    @pl.when(stage == last)
    def _():
        for h in range(heads):
            yin[h] = xout[last, h]

    @pl.when(stage < last)
    def _():
        for h in range(heads):
            exit_copy(0, h).wait_recv()

    final = [yin[h].astype(F32) for h in range(heads)]
    total = sum(jnp.sum(a * a, axis=1, keepdims=True) for a in final)
    part_mine[...] = jnp.broadcast_to(total, part_mine.shape)
    part_copies = [
        pltpu.make_async_remote_copy(
            src_ref=part_mine,
            dst_ref=part_other.at[d - 1],
            send_sem=part_send.at[d - 1],
            recv_sem=part_recv.at[d - 1],
            device_id={"tp": peer(d)},
            device_id_type=MESH,
        )
        for d in others
    ]
    for copy in part_copies:
        copy.start()

    @pl.when(stage > 0)
    def _():
        for h in range(heads):
            if h != early:
                entry_copy(h).wait_send()

    def drain(m, _):
        for h in range(heads):
            for d in others:
                forward_copy(m, d, h).wait_send()

        @pl.when((stage < last) | (m < last))
        def _():
            for h in range(heads):
                next_copy(m, h).wait_send()

        return 0

    lax.fori_loop(0, stages, drain, 0)
    total = part_mine[...]
    for copy in part_copies:
        copy.wait()
    for d in others:
        total = total + part_other[d - 1]
    inv_rms = lax.rsqrt(total / model_width + epsilon)
    for h in range(heads):
        part = slice(h * width, (h + 1) * width)
        out[:, part] = (final[h] * inv_rms * closing_gain[:, part]).astype(BF16)


def on_device(
    stages,
    group,
    tokens,
    query_matrix,
    key_matrix,
    value_matrix,
    output_gate_weight,
    strength_weight,
    decay_input_weight,
    decay_scale_table,
    log_spike_decay,
    head_norm_gain,
    closing_norm_gain,
):
    _, length, half = tokens.shape
    heads = strength_weight.shape[-1]
    width = half // heads

    def rows_of(weight):
        return jnp.pad(weight[0].T, ((0, 1), (0, 0))) if heads == 1 else weight[0].T

    vmem = pl.BlockSpec(memory_space=pltpu.VMEM)
    anywhere = pl.BlockSpec(memory_space=pltpu.HBM)
    dma = pltpu.SemaphoreType.DMA
    result = pl.pallas_call(
        functools.partial(stack_kernel, stages, group),
        out_shape=pltpu.VMEM((length, half), BF16),
        in_specs=[anywhere] * 11,
        out_specs=vmem,
        scratch_shapes=[
            pltpu.VMEM((max(heads, 2), group * half), BF16),
            pltpu.VMEM((max(heads, 2), group * half), BF16),
            pltpu.VMEM((1, heads), F32),
            pltpu.VMEM((heads, length), F32),
            pltpu.VMEM((1, half), F32),
            pltpu.VMEM((1, half), F32),
            pltpu.VMEM((4, group * half, half), BF16),
            pltpu.VMEM((4, length, half), F32),
            pltpu.VMEM((stages, group * heads, length, width), BF16),
            pltpu.VMEM((stages + 1, heads, length, width), BF16),
            pltpu.VMEM((heads, length, width), BF16),
            pltpu.VMEM((length, length), jnp.int32),
            pltpu.VMEM((length, length), F32),
            pltpu.VMEM((length, width), F32),
            pltpu.VMEM((group - 1, length, width), F32),
            dma((4,)),
            dma((6,)),
            dma((heads,)),
            pltpu.SemaphoreType.REGULAR,
            dma((stages, heads)),
            dma((heads,)),
            dma((stages, group - 1, heads)),
            dma((stages, group - 1, heads)),
            dma((stages, heads)),
            dma((heads,)),
            dma((group - 1,)),
            dma((group - 1,)),
        ],
        compiler_params=pltpu.CompilerParams(
            collective_id=0, has_side_effects=True, vmem_limit_bytes=60 * 1024 * 1024
        ),
    )(
        tokens[0],
        query_matrix[0],
        key_matrix[0],
        value_matrix[0],
        output_gate_weight[0],
        rows_of(strength_weight),
        rows_of(decay_input_weight),
        decay_scale_table,
        log_spike_decay[0].T,
        head_norm_gain,
        closing_norm_gain[None],
    )
    return result[None]


def solution(mesh):
    placed = (
        P("pp", "fs", "tp"),
        P("pp", None, "tp"),
        P("pp", None, "tp"),
        P("pp", None, "tp"),
        P("pp", None, "tp"),
        P("pp", None, "tp"),
        P("pp", None, "tp"),
        P("pp", "tp"),
        P("pp", None, "tp"),
        P("pp", "tp"),
        P("tp"),
    )
    return jax.shard_map(
        functools.partial(on_device, mesh.shape["pp"], mesh.shape["tp"]),
        mesh=mesh,
        in_specs=placed,
        out_specs=P("pp", "fs", "tp"),
        check_vma=False,
    )
```
